32 devices in a mesh: fs: 4 (over z), tp: 8 (over y, x, core).
Axes of the slice: x: 2, y: 2, z: 4, core: 2. Of those that a mesh axis runs over, the one named last changes fastest.
Arguments:
- inputs: bfloat16 [1024, 2016], P('fs'), may hold values from -6 to 6
- pre_act: bfloat16 [1024, 4032], P('fs', 'tp'), may hold values from -6 to 6
- cotangent: bfloat16 [1024, 2016], P('fs'), may hold values from -6 to 6
- w_up: bfloat16 [2016, 4032], P('fs', 'tp'), may hold values from -0.125 to 0.125
- w_down: bfloat16 [4032, 2016], P('tp', 'fs'), may hold values from -0.09375 to 0.09375
Outputs:
- grad_input: bfloat16 [1024, 2016], P('fs')
- grad_up: float32 [2016, 4032], P('fs', 'tp')
- grad_down: float32 [4032, 2016], P('tp', 'fs')
The draws below stay inside these ranges and needn't reach their ends.
All inputs are finite; a program needn't handle non-finite values.
Results may differ from the reference program's by a relative error of at most 0.017.
Values may be sent and summed in bfloat16 or wider, within the bound.
A program may use at most 64 MiB of HBM per device.

```python
import jax
import jax.numpy as jnp
from jax import lax

D = 2016
FF = 4032
TOKENS = 1024
N_TP = 8


def strengthened(entries, rng, source, target, blocks, factor):
    def block_of(position):
        return (jnp.arange(entries.shape[position]) // (entries.shape[position] // blocks)).reshape((-1,) + (1,) * (entries.ndim - 1 - position))

    one_side = jax.random.permutation(rng, blocks)[block_of(target)]
    far = (block_of(target) + blocks // 2) % blocks
    return jnp.where((block_of(source) == one_side) | (block_of(source) == far), factor * entries, entries)


def block_levels(stream_key, shape, split, least, largest):
    def one(axis_at, shards_of):
        steps = jax.random.uniform(jax.random.fold_in(jax.random.fold_in(stream_key, 6), axis_at), (shards_of,), jnp.float32, least / len(split), largest / len(split))
        return jnp.repeat(jnp.exp(steps), shape[axis_at] // shards_of).reshape((-1,) + (1,) * (len(shape) - axis_at - 1))

    factor_of = one(*split[0])
    for cut in split[1:]:
        factor_of = factor_of * one(*cut)
    return factor_of


def gaussian(key, extent, spread, limit, cuts=(), dtype=jnp.bfloat16):
    loudness = block_levels(key, extent, cuts, -0.22, 0.18) if cuts else 1.0
    result = jax.random.normal(key, extent, jnp.float32) * spread * loudness
    return jnp.minimum(jnp.maximum(result, -limit), limit).astype(dtype)


def bell_draw_with(stream_key, shape, deviation, most, split, heavy, held_as=jnp.bfloat16):
    result = deviation * jax.random.normal(stream_key, shape, jnp.float32)
    if split:
        result = result * block_levels(stream_key, shape, split, -0.22, 0.18)
    return jnp.clip(strengthened(result, jax.random.fold_in(stream_key, 3), *heavy), -most, most).astype(held_as)


def setup_inputs(seed: int = 0) -> dict:
    key_of = jax.random.split(jax.random.key(seed), 6)
    inputs = bell_draw_with(key_of[0], (TOKENS, D), 1.0, 6.0, ((0, 4),), (0, 1, 4, 2.0))
    pre_act = gaussian(key_of[1], (TOKENS, FF), 1.0, 6.0, ((0, 4), (1, 8)))
    cotangent = bell_draw_with(key_of[2], (TOKENS, D), 1.0, 6.0, ((0, 4),), (0, 1, 4, 2.0))
    w_up = gaussian(key_of[3], (D, FF), D ** -0.5, 0.125, ((0, 4), (1, 8)))
    w_down = gaussian(key_of[4], (FF, D), FF ** -0.5, 0.09375, ((0, 8), (1, 4)))
    return {"inputs": inputs, "pre_act": pre_act, "cotangent": cotangent, "w_up": w_up, "w_down": w_down}


def reference(inputs, pre_act, cotangent, w_up, w_down):
    positive = jnp.maximum(pre_act.astype(jnp.float32), 0.0)
    hidden = (positive * positive).astype(jnp.bfloat16)
    hidden_grad = lax.dot_general(cotangent, w_down, (((1,), (1,)), ((), ())), preferred_element_type=jnp.float32)
    pre_grad = (2.0 * positive * hidden_grad).astype(jnp.bfloat16)
    grad_down = lax.dot_general(hidden, cotangent, (((0,), (0,)), ((), ())), preferred_element_type=jnp.float32)
    grad_up = lax.dot_general(inputs, pre_grad, (((0,), (0,)), ((), ())), preferred_element_type=jnp.float32)
    width = FF // N_TP

    def add_block(index, total):
        start = (index * width).astype(jnp.int32)
        piece_grad = lax.dynamic_slice_in_dim(pre_grad, start, width, 1)
        piece_weight = lax.dynamic_slice_in_dim(w_up, start, width, 1)
        partial_sum = lax.dot_general(piece_grad, piece_weight, (((1,), (1,)), ((), ())), preferred_element_type=jnp.float32).astype(jnp.bfloat16)
        partial_sum = lax.optimization_barrier(partial_sum)
        return total + partial_sum.astype(jnp.float32)

    total = lax.fori_loop(0, N_TP, add_block, jnp.zeros((TOKENS, D), jnp.float32))
    return total.astype(jnp.bfloat16), grad_up, grad_down
```

```python
import functools

import jax
import jax.numpy as jnp
from jax import lax
from jax.experimental import pallas as pl
from jax.experimental.pallas import tpu as pltpu
from jax.sharding import PartitionSpec as P

MESH = pl.DeviceIdType.MESH
F32 = jnp.float32
BF16 = jnp.bfloat16
NT = (((1,), (1,)), ((), ()))
TN = (((0,), (0,)), ((), ()))


def kernel(nf, nt, pieces, inputs, pre_act, cotangent, w_up, w_down, grad_input, grad_up, grad_down,
           cot_split, in_split, cot_all, in_all, pa, pg, hg, rs_out, rs_in, px_out, px_in, keep,
           xy_out, xy_in, zt_out, share,
           a2a_s, a2a_r, ring_s, ring_r, pair_s, pair_r, rs_s, rs_r, ag_s, ag_r,
           px_s, px_r, xy_s, xy_r, zt_s, zt_r, fa_s, fa_r, fd_s, fd_r):
    f, t = lax.axis_index("fs"), lax.axis_index("tp")
    half = nt // 2
    rows, width = pre_act.shape
    part = rows // nt
    block = w_up.shape[0]
    step_rows = rows // pieces
    odd = lax.rem(t, 2)
    partner = t + 1 - 2 * odd
    sent = []

    def copy(src, dst, ssem, rsem, fs=None, tp=None):
        return pltpu.make_async_remote_copy(
            src_ref=src, dst_ref=dst, send_sem=ssem, recv_sem=rsem,
            device_id=(f if fs is None else fs, t if tp is None else tp), device_id_type=MESH,
        )

    def start(desc, cond=None):
        sent.append((cond, desc))
        if cond is None:
            desc.start()
        else:
            pl.when(cond)(desc.start)

    def peer(i):
        return lax.rem(t + 2 * i, nt)

    def source(i):
        return lax.rem(t + nt - 2 * i, nt)

    barrier = pltpu.get_barrier_semaphore()
    for off in range(1, nf):
        pl.semaphore_signal(barrier, inc=1, device_id=(lax.rem(f + off, nf), t), device_id_type=MESH)
    for i in range(1, half):
        pl.semaphore_signal(barrier, inc=1, device_id=(f, peer(i)), device_id_type=MESH)
    pl.semaphore_signal(barrier, inc=1, device_id=(f, partner), device_id_type=MESH)

    def split(src, dst):
        for g in range(nf):
            dst[g] = src[:, g * block:(g + 1) * block].reshape(nt, part, block)

    split(cotangent, cot_split)
    pl.semaphore_wait(barrier, nf - 1 + half)

    def exchange(n, src, dst):
        for off in range(nf - 1, 0, -1):
            g = lax.rem(f + off, nf)
            start(copy(src.at[g, t], dst.at[f, t], a2a_s.at[n, off], a2a_r.at[n, off], fs=g))

    def spread(n, src, dst):
        for off in range(1, nf):
            g = lax.rem(f + nf - off, nf)
            copy(src.at[g, t], dst.at[g, t], a2a_s.at[n, off], a2a_r.at[n, off], fs=g).wait_recv()
            for i in range(1, half):
                start(copy(dst.at[g, t], dst.at[g, t], ring_s.at[n, off, i], ring_r.at[n, off, i], tp=peer(i)))
            start(copy(dst.at[g, t], dst.at[g, t], pair_s.at[n, off, 0], pair_r.at[n, off, 0], tp=partner))

    def relay(n, dst):
        for off in range(1, nf):
            g = lax.rem(f + nf - off, nf)
            for i in range(1, half):
                at = dst.at[g, source(i)]
                copy(at, at, ring_s.at[n, off, i], ring_r.at[n, off, i], tp=source(i)).wait_recv()
                start(copy(at, at, pair_s.at[n, off, i], pair_r.at[n, off, i], tp=partner))

    def collect(n, dst):
        for off in range(1, nf):
            g = lax.rem(f + nf - off, nf)
            for i in range(half):
                at = dst.at[g, lax.rem(partner + nt - 2 * i, nt)]
                copy(at, at, pair_s.at[n, off, i], pair_r.at[n, off, i], tp=partner).wait_recv()

    def nearest(m):
        a = jnp.minimum(f, nf - 1 - f)
        j = (m - 1) // 2
        near = f - 1 - j if m % 2 == 1 else f + 1 + j
        far = jnp.where(f < nf - 1 - f, f + (m - a), f - (m - a))
        return jnp.where(m <= 2 * a, near, far)

    def gather_own(n, buf, s, size):
        at = buf.at[f, pl.ds(s * size, size)]
        start(copy(at, at, ag_s.at[n, 0, 0, s], ag_r.at[n, 0, 0, s], fs=jnp.minimum(f + 1, nf - 1)), f < nf - 1)
        start(copy(at, at, ag_s.at[n, 1, 0, s], ag_r.at[n, 1, 0, s], fs=jnp.maximum(f - 1, 0)), f > 0)

    def gather_next(n, buf, m, s, size):
        g = nearest(m)
        up = g < f
        d = jnp.where(up, 0, 1)
        j = jnp.abs(g - f) - 1
        at = buf.at[g, pl.ds(s * size, size)]
        copy(at, at, ag_s.at[n, d, j, s], ag_r.at[n, d, j, s], fs=jnp.where(up, f - 1, f + 1)).wait_recv()
        to = jnp.where(up, f + 1, f - 1)
        cond = jnp.logical_and(to >= 0, to < nf)
        to = jnp.clip(to, 0, nf - 1)
        k = jnp.minimum(j + 1, nf - 1)
        start(copy(at, at, ag_s.at[n, d, k, s], ag_r.at[n, d, k, s], fs=to), cond)

    exchange(0, cot_split, cot_all)
    pa[f] = pre_act[...]
    gather_own(0, pa, 0, rows)
    split(inputs, in_split)
    cot_all[f] = cot_split[f]
    in_all[f] = in_split[f]
    spread(0, cot_split, cot_all)
    exchange(1, in_split, in_all)
    relay(0, cot_all)
    collect(0, cot_all)

    for g in range(nf):
        hg[g] = lax.dot_general(cot_all[g].reshape(rows, block), w_down[...], NT, preferred_element_type=F32)

    def reduce_step(s, d, g):
        at = pl.ds(s * step_rows, step_rows)
        lower = d == 0
        first = f == 0 if lower else f == nf - 1
        passes = g > f if lower else g < f
        ends = f == g
        to = jnp.minimum(f + 1, nf - 1) if lower else jnp.maximum(f - 1, 0)
        back = jnp.maximum(f - 1, 0) if lower else jnp.minimum(f + 1, nf - 1)
        out = rs_out.at[d, g, at]
        into = rs_in.at[d, g, at]
        arrives = jnp.logical_and(jnp.logical_not(first), jnp.logical_or(passes, ends))

        @pl.when(arrives)
        def _():
            copy(out, into, rs_s.at[d, g, s], rs_r.at[d, g, s], fs=back).wait_recv()
            hg[g, at] = hg[g, at] + rs_in[d, g, at].astype(F32)

        @pl.when(passes)
        def _():
            rs_out[d, g, at] = hg[g, at].astype(BF16)

        start(copy(out, into, rs_s.at[d, g, s], rs_r.at[d, g, s], fs=to), passes)

    for s in range(pieces):
        for k in range(nf):
            reduce_step(s, 0, nf - 1 - k)
            reduce_step(s, 1, k)
        at = pl.ds(s * step_rows, step_rows)
        positive = jnp.maximum(pre_act[at, :].astype(F32), 0.0)
        pg[f, at] = (2.0 * positive * hg[f, at]).astype(BF16)
        gather_own(1, pg, s, step_rows)
        if s == 0:
            gather_next(0, pa, 1, 0, rows)
            spread(1, in_split, in_all)
    for m in range(2, nf):
        gather_next(0, pa, m, 0, rows)

    def term(step, g):
        value = lax.dot_general(pg[g], w_up[...], NT, preferred_element_type=F32).astype(BF16)
        value = value.reshape(half, 2, part, block)

        @pl.when(odd == 0)
        def _():
            keep[step] = value[:, 0]
            px_out[step] = value[:, 1]

        @pl.when(odd == 1)
        def _():
            keep[step] = value[:, 1]
            px_out[step] = value[:, 0]

        start(copy(px_out.at[step], px_in.at[step], px_s.at[step], px_r.at[step], tp=partner))

    def pair_sum(step):
        copy(px_out.at[step], px_in.at[step], px_s.at[step], px_r.at[step], tp=partner).wait_recv()
        xy_out[step] = (keep[step].astype(F32) + px_in[step].astype(F32)).astype(BF16)
        for i in range(1, half):
            start(copy(xy_out.at[step, lax.rem(t // 2 + i, half)], xy_in.at[step, i],
                       xy_s.at[step, i], xy_r.at[step, i], tp=peer(i)))

    def finish(step, g):
        mine = t // 2
        total = keep[step, mine].astype(F32) + px_in[step, mine].astype(F32)
        for i in range(1, half):
            copy(xy_in.at[step, i], xy_in.at[step, i], xy_s.at[step, i], xy_r.at[step, i], tp=source(i)).wait_recv()
            total = total + xy_in[step, i].astype(F32)
        if step == 0:
            share[t, f] = total.astype(BF16)
        else:
            zt_out[step] = total.astype(BF16)
            off = lax.rem(g - f + nf, nf)
            start(copy(zt_out.at[step], share.at[t, f], zt_s.at[off], zt_r.at[off], fs=g))

    order = [f] + [nearest(m) for m in range(1, nf)]
    term(0, f)
    pair_sum(0)
    relay(1, in_all)
    tokens = nf * rows
    for m in range(1, nf):
        for s in range(pieces):
            gather_next(1, pg, m, s, step_rows)
        term(m, order[m])
        pair_sum(m)
        if m == 1:
            positive = jnp.maximum(pa[...].reshape(tokens, width).astype(F32), 0.0)
            hidden = (positive * positive).astype(BF16)
            grad_down[...] = lax.dot_general(
                hidden, cot_all[...].reshape(tokens, block), TN, preferred_element_type=F32)
        finish(m - 1, order[m - 1])
    finish(nf - 1, order[nf - 1])
    collect(1, in_all)
    grad_up[...] = lax.dot_general(
        in_all[...].reshape(tokens, block), pg[...].reshape(tokens, width), TN, preferred_element_type=F32)

    for off in range(1, nf):
        g = lax.rem(f + nf - off, nf)
        copy(zt_out.at[0], share.at[t, g], zt_s.at[off], zt_r.at[off], fs=g).wait_recv()
    for i in range(1, half):
        start(copy(share.at[t], share.at[t], fa_s.at[i], fa_r.at[i], tp=peer(i)))
    start(copy(share.at[t], share.at[t], fd_s.at[0], fd_r.at[0], tp=partner))
    for i in range(1, half):
        at = share.at[source(i)]
        copy(at, at, fa_s.at[i], fa_r.at[i], tp=source(i)).wait_recv()
        start(copy(at, at, fd_s.at[i], fd_r.at[i], tp=partner))
    for i in range(half):
        at = share.at[lax.rem(partner + nt - 2 * i, nt)]
        copy(at, at, fd_s.at[i], fd_r.at[i], tp=partner).wait_recv()
    grad_input[...] = jnp.concatenate(
        [share[:, g].reshape(rows, block) for g in range(nf)], axis=1)

    for cond, desc in sent:
        if cond is None:
            desc.wait_send()
        else:
            pl.when(cond)(desc.wait_send)


def in_kernel(nf, nt, inputs, pre_act, cotangent, w_up, w_down):
    rows, width = pre_act.shape
    block = w_up.shape[0]
    part, half, pieces = rows // nt, nt // 2, 2
    vmem = pl.BlockSpec(memory_space=pltpu.VMEM)
    dma = pltpu.SemaphoreType.DMA
    return pl.pallas_call(
        functools.partial(kernel, nf, nt, pieces),
        out_shape=(
            jax.ShapeDtypeStruct((rows, nf * block), BF16),
            jax.ShapeDtypeStruct((block, width), F32),
            jax.ShapeDtypeStruct((width, block), F32),
        ),
        in_specs=[vmem] * 5,
        out_specs=(vmem,) * 3,
        scratch_shapes=[
            pltpu.VMEM((nf, nt, part, block), BF16),
            pltpu.VMEM((nf, nt, part, block), BF16),
            pltpu.VMEM((nf, nt, part, block), BF16),
            pltpu.VMEM((nf, nt, part, block), BF16),
            pltpu.VMEM((nf, rows, width), BF16),
            pltpu.VMEM((nf, rows, width), BF16),
            pltpu.VMEM((nf, rows, width), F32),
            pltpu.VMEM((2, nf, rows, width), BF16),
            pltpu.VMEM((2, nf, rows, width), BF16),
            pltpu.VMEM((nf, half, part, block), BF16),
            pltpu.VMEM((nf, half, part, block), BF16),
            pltpu.VMEM((nf, half, part, block), BF16),
            pltpu.VMEM((nf, half, part, block), BF16),
            pltpu.VMEM((nf, half, part, block), BF16),
            pltpu.VMEM((nf, part, block), BF16),
            pltpu.VMEM((nt, nf, part, block), BF16),
            dma((2, nf)), dma((2, nf)),
            dma((2, nf, half)), dma((2, nf, half)),
            dma((2, nf, half)), dma((2, nf, half)),
            dma((2, nf, pieces)), dma((2, nf, pieces)),
            dma((2, 2, nf, pieces)), dma((2, 2, nf, pieces)),
            dma((nf,)), dma((nf,)),
            dma((nf, half)), dma((nf, half)),
            dma((nf,)), dma((nf,)),
            dma((half,)), dma((half,)),
            dma((half,)), dma((half,)),
        ],
        compiler_params=pltpu.CompilerParams(
            collective_id=0, has_side_effects=True, vmem_limit_bytes=60 * 1024 * 1024),
    )(inputs, pre_act, cotangent, w_up, w_down)


def on_device(inputs, pre_act, cotangent, w_up, w_down):
    positive = jnp.maximum(pre_act.astype(jnp.float32), 0.0)
    hidden = (positive * positive).astype(jnp.bfloat16)
    columns = cotangent
    hidden_grad = lax.dot_general(
        columns,
        lax.all_gather(w_down, "fs", axis=1, tiled=True),
        (((1,), (1,)), ((), ())),
        preferred_element_type=jnp.float32,
    )
    pre_grad = (2.0 * positive * hidden_grad).astype(jnp.bfloat16)
    columns = inputs
    grad_up = lax.psum_scatter(
        lax.dot_general(
            columns, pre_grad, (((0,), (0,)), ((), ())), preferred_element_type=jnp.float32
        ).astype(jnp.bfloat16),
        "fs",
        scatter_dimension=0,
        tiled=True,
    ).astype(jnp.float32)
    columns = cotangent
    grad_down = (
        lax.psum_scatter(
            lax.dot_general(
                columns, hidden, (((0,), (0,)), ((), ())), preferred_element_type=jnp.float32
            ).astype(jnp.bfloat16),
            "fs",
            scatter_dimension=0,
            tiled=True,
        )
        .astype(jnp.float32)
        .T
    )
    partial_sum = lax.dot_general(
        pre_grad,
        lax.all_gather(w_up, "fs", axis=0, tiled=True),
        (((1,), (1,)), ((), ())),
        preferred_element_type=jnp.float32,
    ).astype(jnp.bfloat16)
    shares = (
        lax.psum_scatter(partial_sum, "tp", scatter_dimension=0, tiled=True)
        .astype(jnp.float32)
        .astype(jnp.bfloat16)
    )
    grad_input = lax.all_gather(shares, "tp", axis=0, tiled=True)
    return (grad_input, grad_up, grad_down)


def solution(mesh):
    in_specs = (P("fs", None), P("fs", "tp"), P("fs", None), P("fs", "tp"), P("tp", "fs"))
    out_specs = (P("fs", None), P("fs", "tp"), P("tp", "fs"))
    nf, nt = mesh.shape["fs"], mesh.shape["tp"]

    def body(inputs, pre_act, cotangent, w_up, w_down):
        rows = pre_act.shape[0]
        if nt % 2 == 0 and nt >= 4 and nf >= 2 and rows % (16 * nt) == 0:
            return in_kernel(nf, nt, inputs, pre_act, cotangent, w_up, w_down)
        return on_device(inputs, pre_act, cotangent, w_up, w_down)

    return jax.shard_map(
        body, mesh=mesh, in_specs=in_specs, out_specs=out_specs, check_vma=False
    )
```

```python
import functools

import jax
import jax.numpy as jnp
from jax import lax
from jax.experimental import pallas as pl
from jax.experimental.pallas import tpu as pltpu
from jax.sharding import PartitionSpec as P

MESH = pl.DeviceIdType.MESH
F32 = jnp.float32
BF16 = jnp.bfloat16
NT = (((1,), (1,)), ((), ()))
NN = (((1,), (0,)), ((), ()))


PIECES = 4


def chunk_of(block, nt):
    return -(-block // (16 * nt)) * 16


def pieces_of(extent, size):
    return [(at, min(size, extent - at)) for at in range(0, extent, size)]


def kernel(nf, nt, size, inputs, pre_act, cotangent, w_up_in, w_down_in, grad_input, grad_up, grad_down,
           cot_split, in_split, cot_all, in_all, pa, pg, hg, w_up, w_down, up_acc, down_acc,
           rs_out, rs_in, px_out, px_in, keep, xy_out, xy_in, zt_out, share,
           a2a_s, a2a_r, ring_s, ring_r, pair_s, pair_r, rs_s, rs_r, ag_s, ag_r,
           px_s, px_r, xy_s, xy_r, zt_s, zt_r, fa_s, fa_r, fd_s, fd_r, load_s):
    f, t = lax.axis_index("fs"), lax.axis_index("tp")
    half = nt // 2
    width, rows = pre_act.shape
    block = w_up.shape[0]
    chunk = cot_all.shape[1] // nt
    cuts = pieces_of(width, size)
    odd = lax.rem(t, 2)
    partner = t + 1 - 2 * odd
    sent = []

    def mine_at(ref, g, c):
        return ref.at[g, pl.ds(pl.multiple_of(c * chunk, chunk), chunk)]

    def copy(src, dst, ssem, rsem, fs=None, tp=None):
        return pltpu.make_async_remote_copy(
            src_ref=src, dst_ref=dst, send_sem=ssem, recv_sem=rsem,
            device_id=(f if fs is None else fs, t if tp is None else tp), device_id_type=MESH,
        )

    def start(desc, cond=None):
        sent.append((cond, desc))
        if cond is None:
            desc.start()
        else:
            pl.when(cond)(desc.start)

    def peer(i):
        return lax.rem(t + 2 * i, nt)

    def source(i):
        return lax.rem(t + nt - 2 * i, nt)

    barrier = pltpu.get_barrier_semaphore()
    for off in range(1, nf):
        pl.semaphore_signal(barrier, inc=1, device_id=(lax.rem(f + off, nf), t), device_id_type=MESH)
    for i in range(1, half):
        pl.semaphore_signal(barrier, inc=1, device_id=(f, peer(i)), device_id_type=MESH)
    pl.semaphore_signal(barrier, inc=1, device_id=(f, partner), device_id_type=MESH)

    loads = []

    def load(src, dst):
        desc = pltpu.make_async_copy(src, dst, load_s.at[len(loads)])
        desc.start()
        loads.append(desc)
        return desc

    def split(src, dst, whole):
        out = [load(src.at[pl.ds(g * block, block)], dst.at[g, pl.ds(0, block)]) for g in range(nf)]
        own = load(src.at[pl.ds(pl.multiple_of(f * block, 8), block)], whole.at[f, pl.ds(0, block)])
        return out, own

    cot_blocks, cot_own = split(cotangent, cot_split, cot_all)
    pa_own = load(pre_act, pa.at[f])
    in_blocks, in_own = split(inputs, in_split, in_all)
    w_down_load = load(w_down_in, w_down)
    w_up_load = load(w_up_in, w_up)
    for desc in cot_blocks:
        desc.wait()
    pl.semaphore_wait(barrier, nf - 1 + half)

    def exchange(n, src, dst):
        for off in range(nf - 1, 0, -1):
            g = lax.rem(f + off, nf)
            start(copy(mine_at(src, g, t), mine_at(dst, f, t), a2a_s.at[n, off], a2a_r.at[n, off], fs=g))

    def spread(n, src, dst):
        for off in range(1, nf):
            g = lax.rem(f + nf - off, nf)
            copy(mine_at(src, g, t), mine_at(dst, g, t), a2a_s.at[n, off], a2a_r.at[n, off], fs=g).wait_recv()
            for i in range(1, half):
                start(copy(mine_at(dst, g, t), mine_at(dst, g, t), ring_s.at[n, off, i], ring_r.at[n, off, i], tp=peer(i)))
            start(copy(mine_at(dst, g, t), mine_at(dst, g, t), pair_s.at[n, off, 0], pair_r.at[n, off, 0], tp=partner))

    def relay(n, dst):
        for off in range(1, nf):
            g = lax.rem(f + nf - off, nf)
            for i in range(1, half):
                at = mine_at(dst, g, source(i))
                copy(at, at, ring_s.at[n, off, i], ring_r.at[n, off, i], tp=source(i)).wait_recv()
                start(copy(at, at, pair_s.at[n, off, i], pair_r.at[n, off, i], tp=partner))

    def collect(n, dst):
        for off in range(1, nf):
            g = lax.rem(f + nf - off, nf)
            for i in range(half):
                at = mine_at(dst, g, lax.rem(partner + nt - 2 * i, nt))
                copy(at, at, pair_s.at[n, off, i], pair_r.at[n, off, i], tp=partner).wait_recv()

    def nearest(m):
        a = jnp.minimum(f, nf - 1 - f)
        j = (m - 1) // 2
        near = f - 1 - j if m % 2 == 1 else f + 1 + j
        far = jnp.where(f < nf - 1 - f, f + (m - a), f - (m - a))
        return jnp.where(m <= 2 * a, near, far)

    def gather_own(n, buf, s, cut):
        at = buf.at[f, pl.ds(*cut)]
        start(copy(at, at, ag_s.at[n, 0, 0, s], ag_r.at[n, 0, 0, s], fs=jnp.minimum(f + 1, nf - 1)), f < nf - 1)
        start(copy(at, at, ag_s.at[n, 1, 0, s], ag_r.at[n, 1, 0, s], fs=jnp.maximum(f - 1, 0)), f > 0)

    def gather_next(n, buf, m, s, cut):
        g = nearest(m)
        up = g < f
        d = jnp.where(up, 0, 1)
        j = jnp.abs(g - f) - 1
        at = buf.at[g, pl.ds(*cut)]
        copy(at, at, ag_s.at[n, d, j, s], ag_r.at[n, d, j, s], fs=jnp.where(up, f - 1, f + 1)).wait_recv()
        to = jnp.where(up, f + 1, f - 1)
        cond = jnp.logical_and(to >= 0, to < nf)
        to = jnp.clip(to, 0, nf - 1)
        k = jnp.minimum(j + 1, nf - 1)
        start(copy(at, at, ag_s.at[n, d, k, s], ag_r.at[n, d, k, s], fs=to), cond)

    exchange(0, cot_split, cot_all)
    pa_own.wait()
    for desc in in_blocks:
        desc.wait()
    spread(0, cot_split, cot_all)
    gather_own(0, pa, 0, (0, width))
    exchange(1, in_split, in_all)
    cot_own.wait()
    in_own.wait()
    w_down_load.wait()
    w_up_load.wait()
    relay(0, cot_all)
    collect(0, cot_all)

    for g in range(nf):
        hg[g] = lax.dot_general(w_down[...], cot_all[g, :block], NN, preferred_element_type=F32)

    def reduce_copy(s, d, g, fs):
        at = pl.ds(*cuts[s])
        return copy(rs_out.at[d, g, at], rs_in.at[d, g, at], rs_s.at[d, g, s], rs_r.at[d, g, s], fs=fs)

    low = f < nf - 1 - f

    def reduce_pass(s, near, k):
        at = pl.ds(*cuts[s])
        up = low if near else jnp.logical_not(low)
        d = jnp.where(up, 0, 1)
        g = jnp.where(up, nf - 1 - k, k)
        to = jnp.clip(jnp.where(up, f + 1, f - 1), 0, nf - 1)
        back = jnp.clip(jnp.where(up, f - 1, f + 1), 0, nf - 1)
        passes = jnp.where(up, g - f, f - g) > 0
        middle = jnp.where(up, f, nf - 1 - f) > 0

        @pl.when(jnp.logical_and(passes, middle))
        def _():
            reduce_copy(s, d, g, back).wait_recv()
            rs_out[d, g, at] = (hg[g, at] + rs_in[d, g, at].astype(F32)).astype(BF16)

        @pl.when(jnp.logical_and(passes, jnp.logical_not(middle)))
        def _():
            rs_out[d, g, at] = hg[g, at].astype(BF16)

        start(reduce_copy(s, d, g, to), passes)

    def reduce_end(s):
        at = pl.ds(*cuts[s])
        for d, there in ((0, f > 0), (1, f < nf - 1)):
            @pl.when(there)
            def _():
                back = jnp.maximum(f - 1, 0) if d == 0 else jnp.minimum(f + 1, nf - 1)
                reduce_copy(s, d, f, back).wait_recv()
                hg[f, at] = hg[f, at] + rs_in[d, f, at].astype(F32)
        positive = jnp.maximum(pa[f, at].astype(F32), 0.0)
        pg[f, at] = (2.0 * positive * hg[f, at]).astype(BF16)
        gather_own(1, pg, s, cuts[s])

    count = len(cuts)
    for s in range(count + 2):
        if s < count:
            for k in range(nf - 1):
                reduce_pass(s, True, k)
        if 1 <= s <= count:
            for k in range(nf - 1):
                reduce_pass(s - 1, False, k)
        if s == 0:
            spread(1, in_split, in_all)
        if s == 1:
            gather_next(0, pa, 1, 0, (0, width))
            relay(1, in_all)
        if s == count and nf > 2:
            gather_next(0, pa, 2, 0, (0, width))
        if s >= 2:
            reduce_end(s - 2)
    for m in range(3, nf):
        gather_next(0, pa, m, 0, (0, width))
    collect(1, in_all)

    def term(step, g):
        value = lax.dot_general(w_up[...], pg[g], NN, preferred_element_type=F32).astype(BF16)
        spare = nt * chunk - block
        if spare:
            value = jnp.concatenate([value, jnp.zeros((spare, rows), BF16)], axis=0)
        value = value.reshape(half, 2, chunk, rows)

        @pl.when(odd == 0)
        def _():
            keep[step] = value[:, 0]
            px_out[step] = value[:, 1]

        @pl.when(odd == 1)
        def _():
            keep[step] = value[:, 1]
            px_out[step] = value[:, 0]

        start(copy(px_out.at[step], px_in.at[step], px_s.at[step], px_r.at[step], tp=partner))
        value = lax.dot_general(in_all[g, :block], pg[g], NT, preferred_element_type=F32)
        up_acc[...] = value if step == 0 else up_acc[...] + value

    def pair_sum(step):
        copy(px_out.at[step], px_in.at[step], px_s.at[step], px_r.at[step], tp=partner).wait_recv()
        xy_out[step] = (keep[step].astype(F32) + px_in[step].astype(F32)).astype(BF16)
        for i in range(1, half):
            start(copy(xy_out.at[step, lax.rem(t // 2 + i, half)], xy_in.at[step, i],
                       xy_s.at[step, i], xy_r.at[step, i], tp=peer(i)))

    def finish(step, g):
        mine = t // 2
        total = keep[step, mine].astype(F32) + px_in[step, mine].astype(F32)
        for i in range(1, half):
            copy(xy_in.at[step, i], xy_in.at[step, i], xy_s.at[step, i], xy_r.at[step, i], tp=source(i)).wait_recv()
            total = total + xy_in[step, i].astype(F32)
        if step == 0:
            share[f, pl.ds(pl.multiple_of(t * chunk, chunk), chunk)] = total.astype(BF16)
        else:
            zt_out[step] = total.astype(BF16)
            off = lax.rem(g - f + nf, nf)
            start(copy(zt_out.at[step], mine_at(share, f, t), zt_s.at[off], zt_r.at[off], fs=g))

    order = [f] + [nearest(m) for m in range(1, nf)]
    term(0, f)
    pair_sum(0)
    for m in range(1, nf):
        for s in range(len(cuts)):
            gather_next(1, pg, m, s, cuts[s])
        term(m, order[m])
        pair_sum(m)
        finish(m - 1, order[m - 1])
    up_store = load(up_acc, grad_up)
    for g in range(nf):
        positive = jnp.maximum(pa[g].astype(F32), 0.0)
        hidden = (positive * positive).astype(BF16)
        value = lax.dot_general(hidden, cot_all[g, :block], NT, preferred_element_type=F32)
        down_acc[...] = value if g == 0 else down_acc[...] + value
    down_store = load(down_acc, grad_down)
    finish(nf - 1, order[nf - 1])

    def stripe(c):
        return share.at[:, pl.ds(pl.multiple_of(c * chunk, chunk), chunk)]

    for off in range(1, nf):
        g = lax.rem(f + nf - off, nf)
        copy(zt_out.at[0], mine_at(share, g, t), zt_s.at[off], zt_r.at[off], fs=g).wait_recv()
    for i in range(1, half):
        start(copy(stripe(t), stripe(t), fa_s.at[i], fa_r.at[i], tp=peer(i)))
    start(copy(stripe(t), stripe(t), fd_s.at[0], fd_r.at[0], tp=partner))
    for i in range(1, half):
        at = stripe(source(i))
        copy(at, at, fa_s.at[i], fa_r.at[i], tp=source(i)).wait_recv()
        start(copy(at, at, fd_s.at[i], fd_r.at[i], tp=partner))
    for i in range(half):
        at = stripe(lax.rem(partner + nt - 2 * i, nt))
        copy(at, at, fd_s.at[i], fd_r.at[i], tp=partner).wait_recv()
    stores = [
        load(share.at[g, pl.ds(0, block)], grad_input.at[pl.ds(g * block, block)]) for g in range(nf)
    ]
    for desc in stores + [down_store, up_store]:
        desc.wait()

    for cond, desc in sent:
        if cond is None:
            desc.wait_send()
        else:
            pl.when(cond)(desc.wait_send)


def in_kernel(nf, nt, inputs, pre_act, cotangent, w_up, w_down):
    rows, width = pre_act.shape
    block = w_up.shape[0]
    half, chunk = nt // 2, chunk_of(block, nt)
    tall = nt * chunk
    size = -(-width // (16 * PIECES)) * 16
    pieces = len(pieces_of(width, size))
    hbm = pl.BlockSpec(memory_space=pl.ANY)
    dma = pltpu.SemaphoreType.DMA
    grad_input, grad_up, grad_down = pl.pallas_call(
        functools.partial(kernel, nf, nt, size),
        out_shape=(
            jax.ShapeDtypeStruct((nf * block, rows), BF16),
            jax.ShapeDtypeStruct((block, width), F32),
            jax.ShapeDtypeStruct((width, block), F32),
        ),
        in_specs=[hbm] * 5,
        out_specs=(hbm,) * 3,
        scratch_shapes=[
            pltpu.VMEM((nf, tall, rows), BF16),
            pltpu.VMEM((nf, tall, rows), BF16),
            pltpu.VMEM((nf, tall, rows), BF16),
            pltpu.VMEM((nf, tall, rows), BF16),
            pltpu.VMEM((nf, width, rows), BF16),
            pltpu.VMEM((nf, width, rows), BF16),
            pltpu.VMEM((nf, width, rows), F32),
            pltpu.VMEM((block, width), BF16),
            pltpu.VMEM((width, block), BF16),
            pltpu.VMEM((block, width), F32),
            pltpu.VMEM((width, block), F32),
            pltpu.VMEM((2, nf, width, rows), BF16),
            pltpu.VMEM((2, nf, width, rows), BF16),
            pltpu.VMEM((nf, half, chunk, rows), BF16),
            pltpu.VMEM((nf, half, chunk, rows), BF16),
            pltpu.VMEM((nf, half, chunk, rows), BF16),
            pltpu.VMEM((nf, half, chunk, rows), BF16),
            pltpu.VMEM((nf, half, chunk, rows), BF16),
            pltpu.VMEM((nf, chunk, rows), BF16),
            pltpu.VMEM((nf, tall, rows), BF16),
            dma((2, nf)), dma((2, nf)),
            dma((2, nf, half)), dma((2, nf, half)),
            dma((2, nf, half)), dma((2, nf, half)),
            dma((2, nf, pieces)), dma((2, nf, pieces)),
            dma((2, 2, nf, pieces)), dma((2, 2, nf, pieces)),
            dma((nf,)), dma((nf,)),
            dma((nf, half)), dma((nf, half)),
            dma((nf,)), dma((nf,)),
            dma((half,)), dma((half,)),
            dma((half,)), dma((half,)),
            dma((3 * nf + 7,)),
        ],
        compiler_params=pltpu.CompilerParams(
            collective_id=0, has_side_effects=True, vmem_limit_bytes=60 * 1024 * 1024),
    )(inputs.T, pre_act.T, cotangent.T, w_up, w_down)
    return grad_input.T, grad_up, grad_down


def on_device(inputs, pre_act, cotangent, w_up, w_down):
    positive = jnp.maximum(pre_act.astype(jnp.float32), 0.0)
    hidden = (positive * positive).astype(jnp.bfloat16)
    columns = cotangent
    hidden_grad = lax.dot_general(
        columns,
        lax.all_gather(w_down, "fs", axis=1, tiled=True),
        (((1,), (1,)), ((), ())),
        preferred_element_type=jnp.float32,
    )
    pre_grad = (2.0 * positive * hidden_grad).astype(jnp.bfloat16)
    columns = inputs
    grad_up = lax.psum_scatter(
        lax.dot_general(
            columns, pre_grad, (((0,), (0,)), ((), ())), preferred_element_type=jnp.float32
        ).astype(jnp.bfloat16),
        "fs",
        scatter_dimension=0,
        tiled=True,
    ).astype(jnp.float32)
    columns = cotangent
    grad_down = (
        lax.psum_scatter(
            lax.dot_general(
                columns, hidden, (((0,), (0,)), ((), ())), preferred_element_type=jnp.float32
            ).astype(jnp.bfloat16),
            "fs",
            scatter_dimension=0,
            tiled=True,
        )
        .astype(jnp.float32)
        .T
    )
    partial_sum = lax.dot_general(
        pre_grad,
        lax.all_gather(w_up, "fs", axis=0, tiled=True),
        (((1,), (1,)), ((), ())),
        preferred_element_type=jnp.float32,
    ).astype(jnp.bfloat16)
    shares = (
        lax.psum_scatter(partial_sum, "tp", scatter_dimension=0, tiled=True)
        .astype(jnp.float32)
        .astype(jnp.bfloat16)
    )
    grad_input = lax.all_gather(shares, "tp", axis=0, tiled=True)
    return (grad_input, grad_up, grad_down)


def solution(mesh):
    in_specs = (P("fs", None), P("fs", "tp"), P("fs", None), P("fs", "tp"), P("tp", "fs"))
    out_specs = (P("fs", None), P("fs", "tp"), P("tp", "fs"))
    nf, nt = mesh.shape["fs"], mesh.shape["tp"]

    def body(inputs, pre_act, cotangent, w_up, w_down):
        rows, width = pre_act.shape
        block = w_up.shape[0]
        tiles = rows % 128 == 0 and width % 8 == 0 and block % 8 == 0
        if tiles and nt % 2 == 0 and nt >= 4 and nf >= 2 and 8 * chunk_of(block, nt) * nt <= 9 * block:
            return in_kernel(nf, nt, inputs, pre_act, cotangent, w_up, w_down)
        return on_device(inputs, pre_act, cotangent, w_up, w_down)

    return jax.shard_map(
        body, mesh=mesh, in_specs=in_specs, out_specs=out_specs, check_vma=False
    )
```
